32 devices in a mesh: ep: 4 (over y, x), tp: 8 (over z, core).
Axes of the slice: x: 2, y: 2, z: 4, core: 2. Of those that a mesh axis runs over, the one named last changes fastest.
Arguments:
- query_latent: bfloat16 [2048, 1024], P('ep'), may hold values from -6 to 6
- joint_latent: bfloat16 [2048, 512], P('ep'), may hold values from -6 to 6
- rotary_key: bfloat16 [2048, 32], P('ep'), may hold values from -60 to 60
- query_gain: float32 [1024], replicated, may hold values from 0.1 to 1.9
- joint_gain: float32 [512], replicated, may hold values from 0.1 to 1.9
- query_weight: bfloat16 [1024, 2048], P(None, 'tp'), may hold values from -0.1875 to 0.1875
- query_rotary: bfloat16 [1024, 1024], P(None, 'tp'), may hold values from -0.1875 to 0.1875
- key_weight: bfloat16 [512, 2048], P(None, 'tp'), may hold values from -0.25 to 0.25
- value_weight: bfloat16 [512, 2048], P(None, 'tp'), may hold values from -0.25 to 0.25
- output_weight: bfloat16 [2048, 2048], P('tp'), may hold values from -6 to 6
- expert_input: bfloat16 [2048, 2048], P('ep'), may hold values from -6 to 6
- expert_gain: float32 [2048], replicated, may hold values from 0.1 to 1.9
- routes: int32 [2048, 2], P('ep'), may hold values from 0 to 7, all different within a row; in each aligned block of 512 rows (0 to 511, 512 to 1023, ...) at most 192 rows name the same one
- route_weight: float32 [2048, 2], P('ep'), may hold values from 0.2 to 1
- gate_weight: bfloat16 [8, 2048, 4096], P('ep', None, 'tp'), may hold values from -0.125 to 0.125
- up_weight: bfloat16 [8, 2048, 4096], P('ep', None, 'tp'), may hold values from -0.125 to 0.125
- down_weight: bfloat16 [8, 4096, 2048], P('ep', 'tp'), may hold values from -0.09375 to 0.09375
Outputs:
- mixer_out: bfloat16 [2048, 2048], P(('ep', 'tp'))
- expert_out: bfloat16 [2048, 2048], P('ep', 'tp')
The draws below stay inside these ranges and needn't reach their ends.
Inputs may be any that keep to these rules, and one draw needn't show every extreme that they name: `routes`: A row names 2 different experts. Among the rows of one device (aligned blocks of 512 rows) no expert is named by more than 192 rows, a bound that some block reaches.
All inputs are finite; a program needn't handle non-finite values.
Results may differ from the reference program's by a relative error of at most 0.019.
The reference program's roundings to bfloat16 on the way count: a program that leaves them out, or rounds other values in their place, can miss the bound.
Values may be sent and summed in bfloat16 or wider, within the bound.
A program may use at most 128 MiB of HBM per device.

```python
import math
import jax
import jax.numpy as jnp
import numpy as np
from jax import lax

D = 2048
HEADS = 32
NOPE = 64
ROPE = 32
VDIM = 64
QL = 1024
KVL = 512
FF = 4096
TOPK = 2
TOK_B_DEV = 512
EXPERTS = 8
TOK_A = 2048
TOK_B = 2048
CAP = 192
N_EP = 4
N_TP = 8


def draw_rotary_key(key, part):
    base = jax.random.normal(jax.random.fold_in(key, 11), (TOK_A, ROPE), jnp.float32)
    return jnp.clip(base, -60.0, 60.0).astype(jnp.bfloat16)


def level_of(stream_key, shape, shards, low, high):
    def one(dim, blocks):
        draws = jax.random.uniform(jax.random.fold_in(jax.random.fold_in(stream_key, 6), dim), (blocks,), jnp.float32, low / len(shards), high / len(shards))
        return jnp.repeat(jnp.exp(draws), shape[dim] // blocks).reshape((-1,) + (1,) * (len(shape) - dim - 1))

    gain = one(*shards[0])
    for cut in shards[1:]:
        gain = gain * one(*cut)
    return gain


def deal_out(rng, own, number, rows, amount, top, most, slope):
    sequence = jax.random.permutation(rng, amount)
    packed, usual = load_shares(amount, rows * top, most, slope, True), load_shares(amount, rows * top, most, slope, False)
    places = jnp.arange(amount)

    def named(sizes, rotation):
        used = int((sizes > 0).sum())
        fixed = max(1, used // 4)
        passed = fixed + (places - fixed + rotation * (used - fixed)) % max(1, amount - fixed)
        return jnp.zeros((amount,), jnp.int32).at[sequence[jnp.where(places < fixed, places, passed)]].set(jnp.asarray(sizes, jnp.int32))

    sizes = jnp.where(number % 4 == 0, named(packed, number // 4), named(usual, number - number // 4 - 1))
    mixed = jax.random.permutation(jax.random.fold_in(own, 3), amount)
    giver, receiver = mixed[0:amount // 2 * 2:2], mixed[1:amount // 2 * 2:2]
    margin = jnp.minimum(sizes[giver] - 1, most - sizes[receiver]) // 2
    margin = jnp.where((giver == sequence[0]) | (receiver == sequence[0]) | (sizes[receiver] == 0), 0, jnp.maximum(margin, 0))
    passed = jax.random.randint(jax.random.fold_in(own, 4), (amount // 2,), 0, 1 << 20) % (margin + 1)
    sizes = sizes.at[giver].add(-passed).at[receiver].add(passed)
    members = jnp.searchsorted(jnp.cumsum(sizes), jnp.arange(rows * top), side="right").astype(jnp.int32)
    listing = members.reshape(top, rows).T
    listing = listing[jax.random.permutation(jax.random.fold_in(own, 1), rows)]
    rotation = jax.random.randint(jax.random.fold_in(own, 2), (rows, 1), 0, top)
    return jnp.take_along_axis(listing, (jnp.arange(top)[None, :] + rotation) % top, axis=1)


def load_shares(count, total, reach, skew, full):
    weights = [(1 << 20) // math.isqrt(grade ** skew) + 1 for grade in range(1, count + 1)]
    largest = reach if full else min(reach, max(-(-total // count), total * weights[0] // sum(weights)))
    least = 1 if total - largest >= count - 1 else 0
    given, rest = [largest] + [least] * (count - 1), total - largest - least * (count - 1)
    while rest > 0:
        free = [i for i in range(1, count) if given[i] < largest] or [i for i in range(1, count) if given[i] < reach]
        mass, remaining = sum([weights[i] for i in free]), rest
        for i in free:
            addition = min(reach - given[i], max(1, remaining * weights[i] // mass), rest)
            given[i] = given[i] + addition
            rest = rest - addition
    return np.array(given)


def gaussian(stream_key, dims, scale, bound, cuts=(), kind=jnp.bfloat16):
    loudness = level_of(stream_key, dims, cuts, -0.22, 0.18) if cuts else 1.0
    result = jax.random.normal(stream_key, dims, jnp.float32) * scale * loudness
    return jnp.minimum(jnp.maximum(result, -bound), bound).astype(kind)


def setup_inputs(seed: int = 0) -> dict:
    keys = jax.random.split(jax.random.key(seed), 18)
    query_latent = gaussian(keys[0], (TOK_A, QL), 1.0, 6.0, ((0, 4),))
    joint_latent = gaussian(keys[1], (TOK_A, KVL), 1.0, 6.0, ((0, 4),))
    rotary_key = draw_rotary_key(jax.random.fold_in(keys[17], 71), 0)
    query_gain = jnp.clip(1.0 + 0.18 * jax.random.normal(keys[3], (QL,), jnp.float32), 0.1, 1.9)
    joint_gain = jnp.clip(1.0 + 0.18 * jax.random.normal(keys[4], (KVL,), jnp.float32), 0.1, 1.9)
    query_weight = gaussian(keys[5], (QL, HEADS * NOPE), QL ** -0.5, 0.1875, ((1, 8),))
    query_rotary = gaussian(keys[6], (QL, HEADS * ROPE), QL ** -0.5, 0.1875, ((1, 8),))
    key_weight = gaussian(keys[7], (KVL, HEADS * NOPE), KVL ** -0.5, 0.25, ((1, 8),))
    value_weight = gaussian(keys[8], (KVL, HEADS * VDIM), KVL ** -0.5, 0.25, ((1, 8),))
    output_weight = gaussian(keys[9], (HEADS * VDIM, D), 1.0, 6.0, ((0, 8),))
    expert_input = gaussian(keys[10], (TOK_B, D), 1.0, 6.0, ((0, 4),))
    expert_gain = jnp.clip(1.0 + 0.18 * jax.random.normal(keys[11], (D,), jnp.float32), 0.1, 1.9)
    routes_keys = jax.random.split(jax.random.fold_in(keys[12], 1), TOK_B // TOK_B_DEV)
    routes_turns = jax.random.permutation(jax.random.fold_in(keys[12], 3), TOK_B // TOK_B_DEV)
    routes = jax.vmap(lambda own, number: deal_out(jax.random.fold_in(keys[12], 2), own, number, TOK_B_DEV, EXPERTS, TOPK, CAP, 1))(routes_keys, routes_turns).reshape((TOK_B, TOPK))
    route_weight = jnp.clip(0.2 + 0.8 * jax.random.uniform(keys[13], (TOK_B, TOPK), jnp.float32) ** level_of(keys[13], (TOK_B, TOPK), ((0, 4),), -0.2, 0.2), 0.2, 1.0)
    gate_weight = gaussian(keys[14], (EXPERTS, D, FF), D ** -0.5, 0.125, ((0, 4), (2, 8)))
    up_weight = gaussian(keys[15], (EXPERTS, D, FF), D ** -0.5, 0.125, ((0, 4), (2, 8)))
    down_weight = gaussian(keys[16], (EXPERTS, FF, D), FF ** -0.5, 0.09375, ((0, 4), (1, 8)))
    return dict(query_latent=query_latent, joint_latent=joint_latent, rotary_key=rotary_key, query_gain=query_gain, joint_gain=joint_gain, query_weight=query_weight, query_rotary=query_rotary, key_weight=key_weight, value_weight=value_weight, output_weight=output_weight, expert_input=expert_input, expert_gain=expert_gain, routes=routes, route_weight=route_weight, gate_weight=gate_weight, up_weight=up_weight, down_weight=down_weight)


NORM_EPSILON = 1e-06
ROTARY_BASE = 10000.0

def norm_rows(source, gain_vector):
    as_float = source.astype(jnp.float32)
    factor = lax.rsqrt(lax.optimization_barrier(jnp.mean(as_float * as_float, axis=-1, keepdims=True)) + NORM_EPSILON)
    return (as_float * factor * gain_vector.astype(jnp.float32)).astype(jnp.bfloat16)

def rotate(source, positions):
    half_width = source.shape[-1] // 2
    frequencies = ROTARY_BASE ** (-jnp.arange(half_width, dtype=jnp.float32) / half_width)
    angles = positions[:, None] * frequencies[None, :]
    view_shape = (source.shape[0],) + (1,) * (source.ndim - 2) + (half_width,)
    cosine_table = jnp.cos(angles).reshape(view_shape)
    sine_table = jnp.sin(angles).reshape(view_shape)
    first_half = source[..., :half_width]
    second = source[..., half_width:]
    return jnp.concatenate([first_half * cosine_table - second * sine_table, second * cosine_table + first_half * sine_table], axis=-1)

def reference(query_latent, joint_latent, rotary_key, query_gain, joint_gain, query_weight, query_rotary, key_weight, value_weight, output_weight, expert_input, expert_gain, routes, route_weight, gate_weight, up_weight, down_weight):
    positions = jnp.arange(TOK_A, dtype=jnp.float32)
    query_normed = norm_rows(query_latent, query_gain)
    joint_normed = norm_rows(joint_latent, joint_gain)
    turned_key = rotate(rotary_key.astype(jnp.float32), positions).astype(jnp.bfloat16)
    query_plain = jnp.dot(query_normed, query_weight, preferred_element_type=jnp.float32).astype(jnp.bfloat16)
    query_plain = query_plain.reshape(TOK_A, HEADS, NOPE)
    query_turned = jnp.dot(query_normed, query_rotary, preferred_element_type=jnp.float32)
    query_turned = rotate(query_turned.reshape(TOK_A, HEADS, ROPE), positions).astype(jnp.bfloat16)
    key_plain = jnp.dot(joint_normed, key_weight, preferred_element_type=jnp.float32).astype(jnp.bfloat16)
    key_plain = key_plain.reshape(TOK_A, HEADS, NOPE)
    values = jnp.dot(joint_normed, value_weight, preferred_element_type=jnp.float32).astype(jnp.bfloat16)
    values = values.reshape(TOK_A, HEADS, VDIM)
    score_scale = (NOPE + ROPE) ** (-0.5)

    def one_head(items_in):
        query_head, turned_head, key_head, value_head = items_in
        scores = jnp.dot(query_head, key_head.T, preferred_element_type=jnp.float32)
        scores = (scores + jnp.dot(turned_head, turned_key.T, preferred_element_type=jnp.float32)) * score_scale
        row_top = lax.optimization_barrier(jnp.max(scores, axis=-1, keepdims=True))
        expo = jnp.exp(scores - row_top)
        row_total = lax.optimization_barrier(jnp.sum(expo, axis=-1, keepdims=True))
        mixed_values = jnp.dot(expo.astype(jnp.bfloat16), value_head, preferred_element_type=jnp.float32)
        return (mixed_values / row_total).astype(jnp.bfloat16)
    per_head = lax.map(one_head, (query_plain.transpose(1, 0, 2), query_turned.transpose(1, 0, 2), key_plain.transpose(1, 0, 2), values.transpose(1, 0, 2)))
    attended = per_head.transpose(1, 0, 2).reshape(TOK_A, HEADS * VDIM)
    mixer_out = jnp.dot(attended, output_weight, preferred_element_type=jnp.float32).astype(jnp.bfloat16)
    expert_normed = norm_rows(expert_input, expert_gain)
    flat_routes = routes.reshape(-1).astype(jnp.int32)
    pair_count = TOK_B * TOPK
    owner_token = jnp.arange(pair_count, dtype=jnp.int32) // TOPK
    onehot = (flat_routes[:, None] == jnp.arange(EXPERTS, dtype=jnp.int32)[None, :]).astype(jnp.int32)
    rank_within = lax.optimization_barrier(jnp.sum((jnp.cumsum(onehot, axis=0) - onehot) * onehot, axis=1)).astype(jnp.int32)
    slot_width = N_EP * CAP
    slot_token = jnp.zeros((EXPERTS, slot_width), jnp.int32).at[flat_routes, rank_within].set(owner_token)
    block_width = FF // N_TP

    def one_expert(items_in):
        token_index, gate_matrix, up_matrix, down_matrix = items_in
        rows_in = expert_normed[token_index]
        gate_acts = jnp.dot(rows_in, gate_matrix, preferred_element_type=jnp.float32)
        up_acts = jnp.dot(rows_in, up_matrix, preferred_element_type=jnp.float32)
        hidden = (jax.nn.silu(gate_acts) * up_acts).astype(jnp.bfloat16)

        def add_block(running, block_index):
            start_at = (block_index * block_width).astype(jnp.int32)
            part_sum = jnp.dot(lax.dynamic_slice_in_dim(hidden, start_at, block_width, 1), lax.dynamic_slice_in_dim(down_matrix, start_at, block_width, 0), preferred_element_type=jnp.float32)
            part_sum = lax.optimization_barrier(part_sum.astype(jnp.bfloat16))
            return (running + part_sum.astype(jnp.float32), None)
        running, _ = lax.scan(add_block, jnp.zeros((slot_width, D), jnp.float32), jnp.arange(N_TP, dtype=jnp.int32))
        return running.astype(jnp.bfloat16)
    results = lax.map(one_expert, (slot_token, gate_weight, up_weight, down_weight))
    picked = results[flat_routes, rank_within].astype(jnp.float32).reshape(TOK_B, TOPK, D)
    expert_out = lax.optimization_barrier(jnp.sum(picked * route_weight[:, :, None], axis=1)).astype(jnp.bfloat16)
    return (mixer_out, expert_out)
```

```python
import functools

import jax
import jax.numpy as jnp
from jax import lax
from jax.experimental import pallas as pl
from jax.experimental.pallas import tpu as pltpu
from jax.sharding import PartitionSpec as P

NOPE = 64
VDIM = 64

NORM_EPSILON = 1e-06
ROTARY_BASE = 10000.0
F32 = jnp.float32
BF16 = jnp.bfloat16


def norm_rows(source, gain_vector):
    as_float = source.astype(F32)
    factor = lax.rsqrt(jnp.mean(as_float * as_float, axis=-1, keepdims=True) + NORM_EPSILON)
    return (as_float * factor * gain_vector).astype(BF16)


def rotation_tables(positions, width, copies):
    half_width = width // 2
    lane = jnp.arange(width * copies, dtype=jnp.int32) % width
    frequencies = ROTARY_BASE ** (-(lane % half_width).astype(F32) / half_width)
    angles = positions[:, None] * frequencies[None, :]
    sign = jnp.where(lane < half_width, -1.0, 1.0).astype(F32)
    return jnp.cos(angles), jnp.sin(angles) * sign[None, :]


def swap_matrix(width, copies):
    half_width = width // 2
    lane = jnp.arange(width * copies, dtype=jnp.int32)
    partner = (lane // width) * width + (lane % width + half_width) % width
    return (lane[:, None] == partner[None, :]).astype(BF16)


def attention_kernel(head_count, turn_width, scale, q_ref, qt_ref, kt_ref, tk_ref, v_ref, out_ref):
    turned_keys = tk_ref[...]
    pieces = []
    per_pair = 128 // VDIM
    for head in range(head_count):
        query = jnp.concatenate(
            [
                q_ref[:, head * NOPE : (head + 1) * NOPE],
                qt_ref[:, head * turn_width : (head + 1) * turn_width],
            ],
            axis=1,
        )
        keys = jnp.concatenate([kt_ref[head * NOPE : (head + 1) * NOPE, :], turned_keys], axis=0)
        scores = jnp.dot(query, keys, preferred_element_type=F32) * scale
        top = jnp.max(scores, axis=-1, keepdims=True)
        expo = jnp.exp(scores - top)
        total = jnp.sum(expo, axis=-1, keepdims=True)
        pair = head // per_pair
        mixed = jnp.dot(
            expo.astype(BF16), v_ref[:, pair * 128 : (pair + 1) * 128], preferred_element_type=F32
        )
        inner = head % per_pair
        mixed = mixed[:, inner * VDIM : (inner + 1) * VDIM]
        pieces.append((mixed / total).astype(BF16))
    out_ref[...] = jnp.concatenate(pieces, axis=1)


def attention(query_plain, query_turned, keys_t, turned_t, values, turn_width):
    rows, width = query_plain.shape
    tokens = values.shape[0]
    head_count = width // NOPE
    block = 128
    scale = (NOPE + turn_width) ** (-0.5)
    whole = lambda i: (0, 0)
    return pl.pallas_call(
        functools.partial(attention_kernel, head_count, turn_width, scale),
        grid=(rows // block,),
        in_specs=[
            pl.BlockSpec((block, width), lambda i: (i, 0)),
            pl.BlockSpec((block, query_turned.shape[1]), lambda i: (i, 0)),
            pl.BlockSpec(keys_t.shape, whole),
            pl.BlockSpec(turned_t.shape, whole),
            pl.BlockSpec(values.shape, whole),
        ],
        out_specs=pl.BlockSpec((block, head_count * VDIM), lambda i: (i, 0)),
        out_shape=jax.ShapeDtypeStruct((rows, head_count * VDIM), BF16),
        compiler_params=pltpu.CompilerParams(vmem_limit_bytes=40 * 1024 * 1024),
        cost_estimate=pl.CostEstimate(
            flops=40 * rows * tokens * head_count * (NOPE + turn_width),
            bytes_accessed=4 * tokens * width,
            transcendentals=rows * tokens * head_count,
        ),
        name="attention",
    )(query_plain, query_turned, keys_t, turned_t, values)


def half_of(source, parity, axis):
    half = source.shape[axis] // 2
    return lax.dynamic_slice_in_dim(source, parity * half, half, axis)


def swap_cores(source):
    size = lax.axis_size("tp")
    return lax.ppermute(source, "tp", [(i, i ^ 1) for i in range(size)])


def latent_part(joint_latent, rotary_key, joint_gain, parity):
    row_count = joint_latent.shape[0]
    turn_width = rotary_key.shape[1]
    positions = (lax.axis_index("ep") * row_count + jnp.arange(row_count, dtype=jnp.int32)).astype(F32)
    normed = half_of(norm_rows(joint_latent, joint_gain), parity, 1)
    cosine, sine = rotation_tables(positions, turn_width, 1)
    swapped = jnp.dot(rotary_key, swap_matrix(turn_width, 1), preferred_element_type=F32)
    turned = (rotary_key.astype(F32) * cosine + swapped * sine).astype(BF16)
    return jnp.concatenate([normed, turned], axis=1)


def token_mixer(
    latent,
    query_latent,
    query_gain,
    query_weight,
    query_rotary,
    key_weight,
    value_weight,
    turn_width,
    parity,
):
    mine, other, turned = latent
    row_count = query_latent.shape[0]
    positions = (lax.axis_index("ep") * row_count + jnp.arange(row_count, dtype=jnp.int32)).astype(F32)
    head_count = key_weight.shape[1] // NOPE
    query_normed = norm_rows(query_latent, query_gain)
    query_plain = jnp.dot(query_normed, query_weight, preferred_element_type=F32).astype(BF16)
    cosine, sine = rotation_tables(positions, turn_width, head_count)
    rotary_swapped = jnp.dot(
        query_rotary, swap_matrix(turn_width, head_count), preferred_element_type=F32
    ).astype(BF16)
    query_turned = (
        jnp.dot(query_normed, query_rotary, preferred_element_type=F32) * cosine
        + jnp.dot(query_normed, rotary_swapped, preferred_element_type=F32) * sine
    ).astype(BF16)

    normed = jnp.where(
        parity == 0,
        jnp.concatenate([mine, other], axis=1),
        jnp.concatenate([other, mine], axis=1),
    )
    keys_t = jnp.einsum("td,df->ft", normed, key_weight, preferred_element_type=F32).astype(BF16)
    values = jnp.dot(normed, value_weight, preferred_element_type=F32).astype(BF16)
    return attention(query_plain, query_turned, keys_t, turned.T, values, turn_width)


def column_blocks(weight, parity, blocks):
    width = weight.shape[2] // blocks
    return jnp.concatenate(
        [
            lax.dynamic_slice_in_dim(weight, (2 * z + parity) * width, width, 2)
            for z in range(blocks // 2)
        ],
        axis=2,
    )


def local(
    query_latent,
    joint_latent,
    rotary_key,
    query_gain,
    joint_gain,
    query_weight,
    query_rotary,
    key_weight,
    value_weight,
    output_weight,
    expert_input,
    expert_gain,
    routes,
    route_weight,
    gate_weight,
    up_weight,
    down_weight,
):
    parity = lax.axis_index("tp") % 2
    tp_size = lax.axis_size("tp")
    row_count, feature_width = expert_input.shape
    group_count = lax.axis_size("ep")
    local_count = gate_weight.shape[0]
    expert_count = local_count * group_count
    capacity = 3 * row_count // (2 * group_count)
    half = feature_width // 2

    part = latent_part(joint_latent, rotary_key, joint_gain, parity)
    part, expert_rows = lax.optimization_barrier((part, expert_input))
    gathered = lax.all_gather(part, "ep", axis=0, tiled=True)

    routes_t = routes.T
    names = jnp.arange(expert_count, dtype=jnp.int32)
    member = (routes_t[0][None, :] == names[:, None]) | (routes_t[1][None, :] == names[:, None])
    token = jnp.arange(row_count, dtype=jnp.int32)
    before = (token[:, None] < token[None, :]).astype(BF16)
    rank = jnp.dot(member.astype(BF16), before, preferred_element_type=F32).astype(jnp.int32)
    place = jnp.where(member, rank, -1)
    slots = jnp.arange(capacity, dtype=jnp.int32)
    chosen = (place[:, None, :] == slots[None, :, None]).astype(BF16)
    chosen = chosen.reshape(expert_count * capacity, row_count)
    rows_half = lax.optimization_barrier(half_of(norm_rows(expert_rows, expert_gain), parity, 1))
    outgoing = jnp.dot(chosen, rows_half, preferred_element_type=F32).astype(BF16)
    outgoing = outgoing.reshape(group_count, local_count, capacity, half)
    mine = lax.all_to_all(outgoing, "ep", split_axis=0, concat_axis=0, tiled=True)
    latent_half = gathered[:, : joint_latent.shape[1] // 2]
    attended = token_mixer(
        (latent_half, swap_cores(latent_half), gathered[:, joint_latent.shape[1] // 2 :]),
        query_latent,
        query_gain,
        query_weight,
        query_rotary,
        key_weight,
        value_weight,
        rotary_key.shape[1],
        parity,
    )
    mine, attended = lax.optimization_barrier((mine, attended))
    other = swap_cores(mine)
    mixer_out = lax.psum_scatter(
        jnp.dot(attended, output_weight, preferred_element_type=F32).astype(BF16),
        "tp",
        scatter_dimension=0,
        tiled=True,
    )

    def project(weight):
        return jnp.einsum(
            "secd,edf->secf", mine, half_of(weight, parity, 1), preferred_element_type=F32
        ) + jnp.einsum(
            "secd,edf->secf", other, half_of(weight, 1 - parity, 1), preferred_element_type=F32
        )

    gate_acts = project(gate_weight)
    up_acts = project(up_weight)
    hidden = (jax.nn.silu(gate_acts) * up_acts).astype(BF16)

    def down(side):
        return jnp.einsum(
            "secf,efd->secd",
            hidden,
            column_blocks(down_weight, side, tp_size),
            preferred_element_type=F32,
        ).astype(BF16)

    theirs = swap_cores(down(1 - parity))
    summed = (down(parity).astype(F32) + theirs.astype(F32)).astype(BF16)
    returned = lax.all_to_all(summed, "ep", split_axis=0, concat_axis=0, tiled=True)
    returned = returned.reshape(expert_count * capacity, half)

    def picked(k):
        slot = jnp.sum(
            jnp.where(routes_t[k][None, :] == names[:, None], names[:, None] * capacity + rank, 0),
            axis=0,
        )
        every = jnp.arange(expert_count * capacity, dtype=jnp.int32)
        pick = (slot[:, None] == every[None, :]).astype(BF16)
        return jnp.dot(pick, returned, preferred_element_type=F32) * route_weight[:, k : k + 1]

    combined = (picked(0) + picked(1)).astype(BF16)
    groups = [list(range(side, tp_size, 2)) for side in range(2)]
    expert_out = lax.psum_scatter(
        combined, "tp", scatter_dimension=1, axis_index_groups=groups, tiled=True
    )
    return (mixer_out, expert_out)


def solution(mesh):
    return jax.shard_map(
        local,
        mesh=mesh,
        in_specs=(
            P("ep", None),
            P("ep", None),
            P("ep", None),
            P(),
            P(),
            P(None, "tp"),
            P(None, "tp"),
            P(None, "tp"),
            P(None, "tp"),
            P("tp", None),
            P("ep", None),
            P(),
            P("ep", None),
            P("ep", None),
            P("ep", None, "tp"),
            P("ep", None, "tp"),
            P("ep", "tp", None),
        ),
        out_specs=(P(("ep", "tp"), None), P("ep", "tp")),
        check_vma=False,
    )
```
